32 devices in a mesh: ep: 8 (over z, x), tp: 4 (over y, core).
Axes of the slice: x: 2, y: 2, z: 4, core: 2. Of those that a mesh axis runs over, the one named last changes fastest.
Arguments:
- queries: bfloat16 [4096, 1024], P('ep', 'tp'), may hold values from -12 to 12
- keys_values: bfloat16 [4096, 8, 128], P('ep', 'tp'), may hold values from -12 to 12
- sink_logits: float32 [16], P('tp'), may hold values from 1 to 7
- out_weight: bfloat16 [1024, 2048], P('tp'), may hold values from -0.5 to 0.5
- expert_input: bfloat16 [4096, 2048], P(('ep', 'tp')), may hold values from -6 to 6
- norm_gain: float32 [2048], replicated, may hold values from 0.1 to 1.9
- route_group: int32 [4096], P(('ep', 'tp')), may hold values from 0 to 3, as said below
- route_expert: int32 [4096, 2], P(('ep', 'tp')), may hold values from 0 to 3, as said below
- group_logits: float32 [4096, 4], P(('ep', 'tp')), may hold values from -6 to 6
- expert_logits: float32 [4096, 2], P(('ep', 'tp')), may hold values from -6 to 6
- gate_weight: bfloat16 [16, 2048, 4096], P('ep', None, 'tp'), may hold values from -0.125 to 0.125
- up_weight: bfloat16 [16, 2048, 4096], P('ep', None, 'tp'), may hold values from -0.125 to 0.125
- down_weight: bfloat16 [16, 4096, 2048], P('ep', 'tp'), may hold values from -0.1875 to 0.1875
Outputs:
- mixed_rows: bfloat16 [4096, 2048], P(('ep', 'tp'))
- expert_mix: bfloat16 [4096, 2048], P(('ep', 'tp'))
The draws below stay inside these ranges and needn't reach their ends.
Inputs may be any that keep to these rules, and one draw needn't show every extreme that they name: `route_group`: among the 128 tokens of one device, every group is named by the same number of tokens. `route_expert`: A token's 2 entries are different members of the group that route_group names; among the 128 tokens of one device, every expert (group and member) is named exactly 16 times.
All inputs are finite; a program needn't handle non-finite values.
Results may differ from the reference program's by a relative error of at most 0.015.
Values may be sent and summed in bfloat16 or wider, within the bound.
A program may use at most 128 MiB of HBM per device.

```python
import jax
import jax.numpy as jnp
from jax import lax

MODEL = 2048
HEADS = 16
KV_HEADS = 8
HEAD_SIZE = 64
WINDOW = 128
GROUPS = 4
CHOSEN = 2
EXPERT_UNITS = 4096
EXPERT_ROWS = 128
EXPERTS = 16
MIXER_TOKENS = 4096
EXPERT_TOKENS = 4096
N_TP = 4


def routing_tables(key):
    blocks = EXPERT_TOKENS // EXPERT_ROWS
    per_group = EXPERTS // GROUPS
    members = EXPERT_ROWS // GROUPS
    cycles = members // per_group
    rank_scores = jax.random.randint(jax.random.fold_in(key, 101), (blocks, EXPERT_ROWS), 0, 1 << 20) * EXPERT_ROWS + jnp.arange(EXPERT_ROWS, dtype=jnp.int32)[None, :]
    ranking = jnp.argsort(rank_scores, axis=1).astype(jnp.int32)
    group_of = ranking % GROUPS
    within = ranking // GROUPS
    order_scores = jax.random.randint(jax.random.fold_in(key, 102), (blocks, GROUPS, per_group), 0, 1 << 20) * per_group + jnp.arange(per_group, dtype=jnp.int32)
    orders = jnp.argsort(order_scores, axis=2).astype(jnp.int32)
    shift_table = 1 + jax.random.randint(jax.random.fold_in(key, 103), (blocks, GROUPS, cycles), 0, per_group - 1)
    block_index = jnp.arange(blocks, dtype=jnp.int32)[:, None]
    shift_by = shift_table[block_index, group_of, within // per_group]
    first_pick = orders[block_index, group_of, within % per_group]
    second = orders[block_index, group_of, (within + shift_by) % per_group]
    return (group_of.reshape(EXPERT_TOKENS), jnp.stack([first_pick, second], axis=-1).reshape(EXPERT_TOKENS, 2))


def draw_route_group(key, part):
    return routing_tables(key)[0].astype(jnp.int32)


def draw_route_expert(key, part):
    return routing_tables(key)[1].astype(jnp.int32)


def draw_queries(key, part):
    base = jnp.clip(jax.random.normal(jax.random.fold_in(key, 11), (MIXER_TOKENS, HEADS * HEAD_SIZE), jnp.float32), -6.0, 6.0)
    return base.astype(jnp.bfloat16)


def draw_keys_values(key, part):
    base = jnp.clip(jax.random.normal(jax.random.fold_in(key, 12), (MIXER_TOKENS, KV_HEADS, 2 * HEAD_SIZE), jnp.float32), -6.0, 6.0)
    return base.astype(jnp.bfloat16)


def block_levels(stream_key, extent, split, smallest, largest):
    level, own = 1.0, jax.random.fold_in(stream_key, 6)
    for position, shards_of in split:
        heights = jnp.exp(jax.random.uniform(jax.random.fold_in(own, position), (shards_of,), jnp.float32, smallest / len(split), largest / len(split)))
        level = level * jnp.repeat(heights, extent[position] // shards_of).reshape([-1 if axis == position else 1 for axis in range(len(extent))])
    return level


def noise(key, extent, deviation, reach, cuts=(), held_as=jnp.bfloat16):
    entries = deviation * jax.random.normal(key, extent, jnp.float32)
    if cuts:
        entries = entries * block_levels(key, extent, cuts, -0.22, 0.18)
    return jnp.clip(entries, -reach, reach).astype(held_as)


def setup_inputs(seed: int = 0) -> dict:
    arg_keys = jax.random.split(jax.random.key(seed), 14)
    return {
        "queries": draw_queries(jax.random.fold_in(arg_keys[13], 71), 0),
        "keys_values": draw_keys_values(jax.random.fold_in(arg_keys[13], 71), 0),
        "sink_logits": jnp.clip(1.0 + 6.0 * jax.random.uniform(arg_keys[2], (HEADS,), jnp.float32) ** block_levels(arg_keys[2], (HEADS,), ((0, 4),), -0.2, 0.2), 1.0, 7.0),
        "out_weight": noise(arg_keys[3], (HEADS * HEAD_SIZE, MODEL), (HEADS * HEAD_SIZE // 8) ** -0.5, 0.5, ((0, 4),)),
        "expert_input": noise(arg_keys[4], (EXPERT_TOKENS, MODEL), 1.0, 6.0, ((0, 32),)),
        "norm_gain": jnp.clip(1.0 + 0.18 * jax.random.normal(arg_keys[5], (MODEL,), jnp.float32), 0.1, 1.9),
        "route_group": draw_route_group(jax.random.fold_in(arg_keys[13], 71), 0),
        "route_expert": draw_route_expert(jax.random.fold_in(arg_keys[13], 71), 0),
        "group_logits": noise(arg_keys[8], (EXPERT_TOKENS, GROUPS), 1.5, 6.0, ((0, 32),), jnp.float32),
        "expert_logits": noise(arg_keys[9], (EXPERT_TOKENS, CHOSEN), 1.0, 6.0, ((0, 32),), jnp.float32),
        "gate_weight": noise(arg_keys[10], (EXPERTS, MODEL, EXPERT_UNITS), MODEL ** -0.5, 0.125, ((0, 8), (2, 4))),
        "up_weight": noise(arg_keys[11], (EXPERTS, MODEL, EXPERT_UNITS), MODEL ** -0.5, 0.125, ((0, 8), (2, 4))),
        "down_weight": noise(arg_keys[12], (EXPERTS, EXPERT_UNITS, MODEL), (EXPERT_UNITS // 4) ** -0.5, 0.1875, ((0, 8), (1, 4))),
    }


norm_eps = 1e-06
masked_score = -1e+30

def attention_part(queries, keys_values, sink_logits):
    sequence = queries.shape[0]
    per_head = HEADS // KV_HEADS
    blocks = sequence // WINDOW
    grouped = queries.reshape(blocks, WINDOW, KV_HEADS, per_head, HEAD_SIZE).transpose(2, 0, 1, 3, 4)
    padded = jnp.pad(keys_values, ((WINDOW, WINDOW), (0, 0), (0, 0)))
    framed = padded.reshape(blocks + 2, WINDOW, KV_HEADS, 2 * HEAD_SIZE)
    nearby = jnp.concatenate([framed[:-2], framed[1:-1], framed[2:]], axis=1).transpose(2, 0, 1, 3)
    query_place = jnp.arange(sequence, dtype=jnp.int32).reshape(blocks, WINDOW)
    key_place = jnp.arange(blocks, dtype=jnp.int32)[:, None] * WINDOW - WINDOW + jnp.arange(3 * WINDOW, dtype=jnp.int32)[None, :]
    distance = jnp.abs(key_place[:, None, :] - query_place[:, :, None])
    allowed = (distance <= WINDOW) & (key_place >= 0)[:, None, :] & (key_place < sequence)[:, None, :]
    head_ids = jnp.arange(HEADS, dtype=jnp.int32).reshape(KV_HEADS, per_head)
    slopes = jnp.exp2(-8.0 * (head_ids + 1).astype(jnp.float32) / HEADS)
    sink_table = sink_logits.reshape(KV_HEADS, per_head)
    penalty_base = distance.astype(jnp.float32)

    def one_head(operands):
        query_part, near_part, slope_part, sink_part = operands
        keys_part = near_part[..., :HEAD_SIZE].astype(jnp.float32)
        value_part = near_part[..., HEAD_SIZE:].astype(jnp.float32)
        scores = jnp.einsum('nqgd,nkd->ngqk', query_part.astype(jnp.float32), keys_part) * HEAD_SIZE ** (-0.5)
        scores = scores - slope_part[None, :, None, None] * penalty_base[:, None]
        scores = jnp.where(allowed[:, None], scores, masked_score)
        sink_column = sink_part[None, :, None]
        highest = jnp.maximum(lax.optimization_barrier(jnp.max(scores, axis=-1)), sink_column)
        exponent = jnp.exp(scores - highest[..., None])
        denominator = lax.optimization_barrier(jnp.sum(exponent, axis=-1)) + jnp.exp(sink_column - highest)
        weights = (exponent / denominator[..., None]).astype(jnp.bfloat16)
        mixed_part = jnp.einsum('ngqk,nkd->nqgd', weights.astype(jnp.float32), value_part)
        return mixed_part.astype(jnp.bfloat16)
    heads_out = lax.map(one_head, (grouped, nearby, slopes, sink_table))
    return heads_out.transpose(1, 2, 0, 3, 4).reshape(sequence, HEADS * HEAD_SIZE)

def normalize(row_block, norm_gain):
    values = row_block.astype(jnp.float32)
    scale = lax.rsqrt(lax.optimization_barrier(jnp.mean(values * values, axis=-1, keepdims=True)) + norm_eps)
    return (values * scale * norm_gain).astype(jnp.bfloat16)

def slot_places(expert_ids, experts, capacity):
    flat_ids = expert_ids.reshape(-1)
    onehot = (flat_ids[:, None] == jnp.arange(experts, dtype=jnp.int32)[None, :]).astype(jnp.int32)
    earlier = jnp.cumsum(onehot, axis=0) - onehot
    return flat_ids * capacity + lax.optimization_barrier(jnp.sum(onehot * earlier, axis=1))

def expert_part(expert_input, norm_gain, route_group, route_expert, group_logits, expert_logits, gate_weight, up_weight, down_weight):
    token_count = expert_input.shape[0]
    experts = gate_weight.shape[0]
    members = experts // GROUPS
    capacity = EXPERT_ROWS * CHOSEN // experts
    blocks = token_count // EXPERT_ROWS
    normed = normalize(expert_input, norm_gain)
    expert_ids = route_group[:, None] * members + route_expert

    def place_block(block_ids):
        return slot_places(block_ids, experts, capacity)
    places = jax.vmap(place_block)(expert_ids.reshape(blocks, EXPERT_ROWS, CHOSEN))
    owners = jnp.repeat(jnp.arange(token_count, dtype=jnp.int32), CHOSEN).reshape(blocks, -1)
    block_index = jnp.arange(blocks, dtype=jnp.int32)[:, None]
    table = jnp.zeros((blocks, experts * capacity), jnp.int32).at[block_index, places].set(owners)
    table = table.reshape(blocks, experts, capacity).transpose(1, 0, 2).reshape(experts, blocks * capacity)
    slice_width = EXPERT_UNITS // N_TP

    def one_expert(operands):
        row_index, gate_part, up_part, down_part = operands
        chosen_rows = jnp.take(normed, row_index, axis=0)
        gate_act = jnp.dot(chosen_rows, gate_part, preferred_element_type=jnp.float32)
        up_act = jnp.dot(chosen_rows, up_part, preferred_element_type=jnp.float32)
        hidden_act = (jax.nn.silu(gate_act) * up_act).astype(jnp.bfloat16)
        running = jnp.zeros((row_index.shape[0], down_part.shape[1]), jnp.float32)
        for slice_index in range(N_TP):
            lower = slice_index * slice_width
            partial_sum = jnp.dot(hidden_act[:, lower:lower + slice_width], down_part[lower:lower + slice_width], preferred_element_type=jnp.float32)
            running = running + lax.optimization_barrier(partial_sum.astype(jnp.bfloat16)).astype(jnp.float32)
        return running.astype(jnp.bfloat16)
    results = lax.map(one_expert, (table, gate_weight, up_weight, down_weight))
    flat_places = places.reshape(token_count, CHOSEN)
    column = (jnp.arange(token_count, dtype=jnp.int32) // EXPERT_ROWS)[:, None] * capacity + flat_places % capacity
    gathered = results[expert_ids, column]
    group_exp = jnp.exp(group_logits)
    picked = lax.optimization_barrier(jnp.sum(jnp.where(jnp.arange(GROUPS, dtype=jnp.int32)[None, :] == route_group[:, None], group_exp, 0.0), axis=1)) / lax.optimization_barrier(jnp.sum(group_exp, axis=1))
    member_exp = jnp.exp(expert_logits)
    route_weight = member_exp / lax.optimization_barrier(jnp.sum(member_exp, axis=1, keepdims=True)) * picked[:, None]
    return lax.optimization_barrier(jnp.sum(route_weight[:, :, None] * gathered.astype(jnp.float32), axis=1)).astype(jnp.bfloat16)

def reference(queries, keys_values, sink_logits, out_weight, expert_input, norm_gain, route_group, route_expert, group_logits, expert_logits, gate_weight, up_weight, down_weight):
    attended = attention_part(queries, keys_values, sink_logits)
    mixed_rows = jnp.dot(attended, out_weight, preferred_element_type=jnp.float32).astype(jnp.bfloat16)
    expert_mix = expert_part(expert_input, norm_gain, route_group, route_expert, group_logits, expert_logits, gate_weight, up_weight, down_weight)
    return (mixed_rows, expert_mix)
```

```python
import jax
import jax.numpy as jnp
from jax import lax
from jax.experimental import pallas as pl
from jax.experimental.pallas import tpu as pltpu
from jax.sharding import PartitionSpec as P
import functools

HEADS = 16
WINDOW = 128
GROUPS = 4


norm_eps = 1e-06
masked_score = -1e30


def extended(cells, sides, width):
    for axis, dim in sides:
        count = lax.axis_size(axis)
        ends = count - 1
        head = lax.slice_in_dim(cells, 0, width, axis=dim)
        tail = lax.slice_in_dim(cells, cells.shape[dim] - width, cells.shape[dim], axis=dim)
        cells = jnp.concatenate(
            [
                lax.ppermute(tail, axis, [(i, (i + 1) % count) for i in range(ends)]),
                cells,
                lax.ppermute(head, axis, [((i + 1) % count, i) for i in range(ends)]),
            ],
            axis=dim,
        )
    return cells


MESH = pl.DeviceIdType.MESH
CORES = 2
META = 128
HI = 32
LO = 64


def expert_kernel(
    dims, x_ref, gain_ref, sel_ref, meta_ref, wg_hbm, wu_hbm, wd_hbm, out_ref,
    wg, wu, wd, sbuf, buf, cbuf, xbuf, hbuf, wrow, pbuf, fb, sb, fin, ret,
    wsem, lsem, zs, zr, gs, gr, ps, pr, fs, fr, ss, sr, bs, br,
):
    planes, ranks, rows, per_block = dims
    tokens, width = x_ref.shape
    local = wg.shape[0]
    units = wg.shape[2]
    per_group = tokens // planes
    sides = rows
    ep, tp = lax.axis_index("ep"), lax.axis_index("tp")
    g, x = ep // ranks, ep % ranks
    y, c = tp // CORES, tp % CORES
    other = 1 - c
    part = pl.ds(0, width)

    def device(g_, x_, y_, c_):
        return (g_ * ranks + x_, y_ * CORES + c_)

    def x_peer(i):
        return lax.rem(x + i, ranks)

    def y_peer(j):
        return lax.rem(y + j, sides)

    loads = []
    for k, (h, v) in enumerate(((wg_hbm, wg), (wu_hbm, wu), (wd_hbm, wd))):
        cp = pltpu.make_async_copy(h, v, wsem.at[k])
        cp.start()
        loads.append(cp)

    barrier = pltpu.get_barrier_semaphore()
    friends = [device(lax.rem(g + d, planes), x, y, c) for d in range(1, planes)]
    friends += [device(g, x_peer(i), y, c) for i in range(1, ranks)]
    friends += [device(g, x, y_peer(j), c) for j in range(1, sides)]
    friends += [device(g, x, y, other)]
    for f in friends:
        pl.semaphore_signal(barrier, inc=1, device_id=f, device_id_type=MESH)

    values = x_ref[...].astype(jnp.float32)
    scale = lax.rsqrt(jnp.mean(values * values, axis=-1, keepdims=True) + norm_eps)
    normed = (values * scale * gain_ref[...]).astype(jnp.bfloat16)
    sel = sel_ref[...]
    ordered = jnp.dot(sel, normed, preferred_element_type=jnp.float32).astype(jnp.bfloat16)
    sbuf[:, :, :width] = ordered.reshape(planes, per_group, width)
    extra = jnp.dot(sel, meta_ref[...], preferred_element_type=jnp.float32).astype(jnp.bfloat16)
    sbuf[:, :, width:] = extra.reshape(planes, per_group, META)

    pl.semaphore_wait(barrier, len(friends))

    def remote(src, dst, s, r, dev):
        cp = pltpu.make_async_remote_copy(
            src_ref=src, dst_ref=dst, send_sem=s, recv_sem=r, device_id=dev, device_id_type=MESH
        )
        cp.start()
        return cp

    sent = []
    for d in range(1, planes):
        to = lax.rem(g + d, planes)
        sent.append(
            remote(sbuf.at[to], buf.at[d, c, x, y], zs.at[d], zr.at[d], device(to, x, y, c))
        )
    own = pltpu.make_async_copy(sbuf.at[g], buf.at[0, c, x, y], lsem)
    own.start()
    own.wait()

    counter = [0]

    def pass_on(d, bx, by, dev):
        block = buf.at[d, c, bx, by]
        sent.append(remote(block, block, gs.at[counter[0]], gr.at[d, c, bx, by], dev))
        counter[0] += 1

    def landed(d, bc, bx, by):
        block = buf.at[d, bc, bx, by]
        pltpu.make_async_remote_copy(
            src_ref=block, dst_ref=block, send_sem=gs.at[0], recv_sem=gr.at[d, bc, bx, by],
            device_id=device(g, x, y, other), device_id_type=MESH,
        ).wait_recv()

    def to_x(d, bx, by):
        for i in range(1, ranks):
            pass_on(d, bx, by, device(g, x_peer(i), y, c))

    def to_y(d, bx, by):
        for j in range(1, sides):
            pass_on(d, bx, by, device(g, x, y_peer(j), c))

    def to_core(d, bx, by):
        pass_on(d, bx, by, device(g, x, y, other))

    def spread(d):
        if d > 0:
            sent[d - 1].wait_recv()
        to_x(d, x, y)
        to_y(d, x, y)
        to_core(d, x, y)

    def relay(d):
        for i in range(1, ranks):
            landed(d, c, x_peer(i), y)
            if d % 2 == 0:
                to_y(d, x_peer(i), y)
            to_core(d, x_peer(i), y)
        for j in range(1, sides):
            landed(d, c, x, y_peer(j))
            if d % 2 == 1:
                to_x(d, x, y_peer(j))
            to_core(d, x, y_peer(j))

    def relay_far(d):
        for i in range(1, ranks):
            for j in range(1, sides):
                landed(d, c, x_peer(i), y_peer(j))
                to_core(d, x_peer(i), y_peer(j))

    def complete(d):
        for bx in range(ranks):
            for by in range(sides):
                landed(d, other, bx, by)

    spread(0)
    for d in range(1, planes):
        spread(d)
        relay(d - 1)
        if d > 1:
            relay_far(d - 2)
    relay(planes - 1)
    relay_far(planes - 2)
    relay_far(planes - 1)
    for d in range(planes):
        complete(d)
    for cp in sent:
        cp.wait_send()
    for cp in loads:
        cp.wait()

    count = CORES * ranks * sides
    many = count * per_group
    slots = count * per_block
    stage = 2

    def gather_rows(first):
        ri = lax.broadcasted_iota(jnp.int32, (many, many), 0)
        ci = lax.broadcasted_iota(jnp.int32, (many, many), 1)
        lower = ((ci < ri) & (ci // per_group == ri // per_group)).astype(jnp.bfloat16)
        lane = lax.broadcasted_iota(jnp.int32, (many, META), 1)
        base = lax.broadcasted_iota(jnp.int32, (many, 1), 0) // per_group * per_block
        slot = lax.broadcasted_iota(jnp.int32, (many, slots), 1).astype(jnp.float32)
        lane_r = lax.broadcasted_iota(jnp.int32, (slots, META), 1)
        for s in range(stage):
            block = buf[first + s].reshape(many, width + META)
            marks = block[:, width:]
            ranks_in = jnp.dot(lower, marks, preferred_element_type=jnp.float32)
            for e in range(local):
                member = x * local + e
                mine = lane == member
                chosen = jnp.sum(jnp.where(mine, marks.astype(jnp.float32), 0.0), axis=1, keepdims=True)
                place = jnp.sum(jnp.where(mine, ranks_in, 0.0), axis=1, keepdims=True)
                place = place + base.astype(jnp.float32)
                hot = jnp.where((place == slot) & (chosen > 0.5), 1.0, 0.0).astype(jnp.bfloat16)
                cbuf[s, e] = hot
                picked = lax.dot_general(
                    hot, block, (((0,), (0,)), ((), ())), preferred_element_type=jnp.float32
                )
                xbuf[e, pl.ds(s * slots, slots), :] = picked[:, :width].astype(jnp.bfloat16)
                tail = picked[:, width:]
                weight = jnp.sum(
                    jnp.where((lane_r == member + HI) | (lane_r == member + LO), tail, 0.0),
                    axis=1, keepdims=True,
                )
                wrow[e, pl.ds(s * slots, slots), :] = jnp.broadcast_to(weight, (slots, META))

    tile = 256

    def hidden_of(e):
        @pl.loop(0, units // tile)
        def _(k):
            cols = pl.ds(pl.multiple_of(k * tile, tile), tile)
            xs = xbuf[e]
            a = jnp.dot(xs, wg[e, :, cols], preferred_element_type=jnp.float32)
            b = jnp.dot(xs, wu[e, :, cols], preferred_element_type=jnp.float32)
            act = a / (1.0 + jnp.exp(-a)) * b * wrow[e, :, :1]
            hbuf[e, :, cols] = act.astype(jnp.bfloat16)

    def project(first):
        @pl.loop(0, width // tile)
        def _(k):
            cols = pl.ds(pl.multiple_of(k * tile, tile), tile)
            outs = [
                jnp.dot(hbuf[e], wd[e, :, cols], preferred_element_type=jnp.float32).astype(jnp.bfloat16)
                for e in range(local)
            ]
            for s in range(stage):
                total = jnp.zeros((many, tile), jnp.float32)
                for e in range(local):
                    total += jnp.dot(
                        cbuf[s, e], outs[e][s * slots : (s + 1) * slots],
                        preferred_element_type=jnp.float32,
                    )
                buf[first + s, :, :, :, :, cols] = total.astype(jnp.bfloat16).reshape(
                    CORES, ranks, sides, per_group, tile
                )

    back = []
    pair, first_hop, second_hop, home = {}, {}, {}, {}

    def swap_cores(d):
        pair[d] = remote(
            buf.at[d, other, :, :, :, part], pbuf.at[d], ps.at[d], pr.at[d], device(g, x, y, other)
        )

    def hop_one(d):
        pair[d].wait_recv()
        for bx in range(ranks):
            for by in range(sides):
                buf[d, c, bx, by, :, part] = (
                    buf[d, c, bx, by, :, part].astype(jnp.float32) + pbuf[d, bx, by].astype(jnp.float32)
                ).astype(jnp.bfloat16)
        first_hop[d] = []
        along_y = d % 2 == 0
        for j in range(1, sides if along_y else ranks):
            for q in range(ranks if along_y else sides):
                if along_y:
                    src, dev = buf.at[d, c, q, y_peer(j), :, part], device(g, x, y_peer(j), c)
                else:
                    src, dev = buf.at[d, c, x_peer(j), q, :, part], device(g, x_peer(j), y, c)
                first_hop[d].append(
                    remote(src, fb.at[d, j - 1, q], fs.at[d, j - 1, q], fr.at[d, j - 1, q], dev)
                )

    def hop_two(d):
        for cp in first_hop[d]:
            cp.wait_recv()
        along_y = d % 2 == 0
        for q in range(ranks if along_y else sides):
            here = (d, c, q, y) if along_y else (d, c, x, q)
            total = buf[(*here, slice(None), part)].astype(jnp.float32)
            for j in range(1, sides if along_y else ranks):
                total += fb[d, j - 1, q].astype(jnp.float32)
            buf[(*here, slice(None), part)] = total.astype(jnp.bfloat16)
        second_hop[d] = []
        for i in range(1, ranks if along_y else sides):
            if along_y:
                src, dev = buf.at[d, c, x_peer(i), y, :, part], device(g, x_peer(i), y, c)
            else:
                src, dev = buf.at[d, c, x, y_peer(i), :, part], device(g, x, y_peer(i), c)
            second_hop[d].append(remote(src, sb.at[d, i - 1], ss.at[d, i - 1], sr.at[d, i - 1], dev))

    def go_home(d):
        for cp in second_hop[d]:
            cp.wait_recv()
        total = buf[d, c, x, y, :, part].astype(jnp.float32)
        for i in range(len(second_hop[d])):
            total += sb[d, i].astype(jnp.float32)
        if d == 0:
            ret[g] = total.astype(jnp.bfloat16)
        else:
            fin[d] = total.astype(jnp.bfloat16)
            to = lax.rem(g + planes - d, planes)
            home[d] = remote(fin.at[d], ret.at[g], bs.at[d], br.at[d], device(to, x, y, c))

    for first in range(0, planes, stage):
        ds = range(first, first + stage)
        before = range(first - stage, first) if first else ()
        gather_rows(first)
        for d in before:
            hop_one(d)
        for e in range(local):
            hidden_of(e)
            if e == 0:
                for d in before:
                    hop_two(d)
        for d in before:
            go_home(d)
        project(first)
        for d in ds:
            swap_cores(d)
    for d in ds:
        hop_one(d)
    for d in ds:
        hop_two(d)
    for d in ds:
        go_home(d)
    for d in range(planes):
        pair[d].wait_send()
        for cp in first_hop[d] + second_hop[d]:
            cp.wait_send()
    for d in range(1, planes):
        home[d].wait_send()
        came = lax.rem(g + d, planes)
        pltpu.make_async_remote_copy(
            src_ref=fin.at[d], dst_ref=ret.at[came], send_sem=bs.at[d], recv_sem=br.at[d],
            device_id=device(came, x, y, c), device_id_type=MESH,
        ).wait_recv()
    out_ref[...] = lax.dot_general(
        sel_ref[...], ret[...].reshape(tokens, width), (((0,), (0,)), ((), ())),
        preferred_element_type=jnp.float32,
    ).astype(jnp.bfloat16)


def expert_mix_of(
    expert_input, norm_gain, route_group, route_expert, group_logits, expert_logits,
    gate_weight, up_weight, down_weight,
):
    ep_size, tp_size = lax.axis_size("ep"), lax.axis_size("tp")
    tokens, width = expert_input.shape
    local, _, units = gate_weight.shape
    planes, ranks, sides = GROUPS, ep_size // GROUPS, tp_size // CORES
    members = local * ranks
    per_group = tokens // planes
    chosen = route_expert.shape[1]
    per_block = per_group * chosen // members
    slots = CORES * ranks * sides * per_block
    many = CORES * ranks * sides * per_group
    ids = jnp.arange(tokens, dtype=jnp.int32)
    same = (route_group[:, None] == route_group[None, :]) & (ids[:, None] < ids[None, :])
    place = route_group * per_group + jnp.sum(same.astype(jnp.int32), axis=0)
    sel = (place[None, :] == ids[:, None]).astype(jnp.bfloat16)
    group_exp = jnp.exp(group_logits)
    groups = jnp.arange(GROUPS, dtype=jnp.int32)[None, :]
    picked = jnp.sum(jnp.where(groups == route_group[:, None], group_exp, 0.0), axis=1) / jnp.sum(
        group_exp, axis=1
    )
    member_exp = jnp.exp(expert_logits)
    weight = member_exp / jnp.sum(member_exp, axis=1, keepdims=True) * picked[:, None]
    high = lax.reduce_precision(weight, 8, 7)
    low = weight - high
    lane = jnp.arange(META, dtype=jnp.int32)[None, :]
    meta = jnp.zeros((tokens, META), jnp.float32)
    for k in range(chosen):
        at = route_expert[:, k : k + 1]
        meta = meta + jnp.where(lane == at, 1.0, 0.0)
        meta = meta + jnp.where(lane == at + HI, high[:, k : k + 1], 0.0)
        meta = meta + jnp.where(lane == at + LO, low[:, k : k + 1], 0.0)
    bf16, dma = jnp.bfloat16, pltpu.SemaphoreType.DMA
    most, wide = max(ranks, sides), max(ranks, sides, 2) - 1
    sends = planes * (ranks * sides * 3)
    vmem = pl.BlockSpec(memory_space=pltpu.VMEM)
    hbm = pl.BlockSpec(memory_space=pl.ANY)
    rows = 2 * slots
    return pl.pallas_call(
        functools.partial(expert_kernel, (planes, ranks, sides, per_block)),
        out_shape=jax.ShapeDtypeStruct((tokens, width), bf16),
        in_specs=[vmem] * 4 + [hbm] * 3,
        out_specs=vmem,
        scratch_shapes=[
            pltpu.VMEM(gate_weight.shape, bf16),
            pltpu.VMEM(up_weight.shape, bf16),
            pltpu.VMEM(down_weight.shape, bf16),
            pltpu.VMEM((planes, per_group, width + META), bf16),
            pltpu.VMEM((planes, CORES, ranks, sides, per_group, width + META), bf16),
            pltpu.VMEM((2, local, many, slots), bf16),
            pltpu.VMEM((local, rows, width), bf16),
            pltpu.VMEM((local, rows, units), bf16),
            pltpu.VMEM((local, rows, META), jnp.float32),
            pltpu.VMEM((planes, ranks, sides, per_group, width), bf16),
            pltpu.VMEM((planes, wide, most, per_group, width), bf16),
            pltpu.VMEM((planes, wide, per_group, width), bf16),
            pltpu.VMEM((planes, per_group, width), bf16),
            pltpu.VMEM((planes, per_group, width), bf16),
            dma((3,)), dma,
            dma((planes,)), dma((planes,)),
            dma((sends,)), dma((planes, CORES, ranks, sides)),
            dma((planes,)), dma((planes,)),
            dma((planes, wide, most)), dma((planes, wide, most)),
            dma((planes, wide)), dma((planes, wide)),
            dma((planes,)), dma((planes,)),
        ],
        compiler_params=pltpu.CompilerParams(
            collective_id=0, has_side_effects=True, vmem_limit_bytes=KERNEL_VMEM
        ),
        cost_estimate=pl.CostEstimate(
            flops=6 * 2 * rows * local * width * units, bytes_accessed=6 * local * width * units, transcendentals=0
        ),
    )(expert_input, norm_gain[None, :], sel, meta.astype(bf16), gate_weight, up_weight, down_weight)


KERNEL_VMEM = 66_000_000


def attend(queries, keys_values, sink_logits):
    row_count = queries.shape[0]
    head_size = keys_values.shape[2] // 2
    kv_local = keys_values.shape[1]
    query_local = queries.shape[1] // head_size
    per_head = query_local // kv_local
    blocks = row_count // WINDOW
    padded = extended(keys_values, (("ep", 0),), WINDOW)
    framed = padded.reshape(blocks + 2, WINDOW, kv_local, 2 * head_size)
    nearby = jnp.concatenate([framed[:-2], framed[1:-1], framed[2:]], axis=1)
    grouped = queries.reshape(blocks, WINDOW, kv_local, per_head, head_size)
    scores = jnp.einsum(
        "nqhgd,nkhd->nhgqk", grouped, nearby[..., :head_size], preferred_element_type=jnp.float32
    ) * head_size ** (-0.5)
    first_row = lax.axis_index("ep") * row_count
    sequence = row_count * lax.axis_size("ep")
    query_place = first_row + jnp.arange(row_count, dtype=jnp.int32).reshape(blocks, WINDOW)
    key_place = (
        first_row
        + jnp.arange(blocks, dtype=jnp.int32)[:, None] * WINDOW
        - WINDOW
        + jnp.arange(3 * WINDOW, dtype=jnp.int32)[None, :]
    )
    distance = jnp.abs(key_place[:, None, :] - query_place[:, :, None])
    allowed = (
        (distance <= WINDOW) & (key_place >= 0)[:, None, :] & (key_place < sequence)[:, None, :]
    )
    head_ids = lax.axis_index("tp") * query_local + jnp.arange(
        query_local, dtype=jnp.int32
    ).reshape(kv_local, per_head)
    slopes = jnp.exp2(-8.0 * (head_ids + 1).astype(jnp.float32) / HEADS)
    scores = scores - slopes[None, :, :, None, None] * distance[:, None, None].astype(jnp.float32)
    scores = jnp.where(allowed[:, None, None], scores, masked_score)
    sink_column = sink_logits.reshape(kv_local, per_head)[None, :, :, None]
    highest = jnp.maximum(jnp.max(scores, axis=-1), sink_column)
    exponent = jnp.exp(scores - highest[..., None])
    denominator = jnp.sum(exponent, axis=-1) + jnp.exp(sink_column - highest)
    weights = (exponent / denominator[..., None]).astype(jnp.bfloat16)
    mixed_part = jnp.einsum(
        "nhgqk,nkhd->nqhgd", weights, nearby[..., head_size:], preferred_element_type=jnp.float32
    )
    return mixed_part.astype(jnp.bfloat16).reshape(row_count, query_local * head_size)


def body(
    queries,
    keys_values,
    sink_logits,
    out_weight,
    expert_input,
    norm_gain,
    route_group,
    route_expert,
    group_logits,
    expert_logits,
    gate_weight,
    up_weight,
    down_weight,
):
    attended = attend(queries, keys_values, sink_logits)
    segment = attended
    mixed_rows = lax.psum_scatter(
        jnp.dot(segment, out_weight, preferred_element_type=jnp.float32).astype(jnp.bfloat16),
        "tp",
        scatter_dimension=0,
        tiled=True,
    )
    expert_mix = expert_mix_of(
        expert_input, norm_gain, route_group, route_expert, group_logits, expert_logits,
        gate_weight, up_weight, down_weight,
    )
    return (mixed_rows, expert_mix)


def solution(mesh):
    placed = (
        P("ep", "tp"),
        P("ep", "tp", None),
        P("tp"),
        P("tp", None),
        P(("ep", "tp"), None),
        P(),
        P(("ep", "tp")),
        P(("ep", "tp"), None),
        P(("ep", "tp"), None),
        P(("ep", "tp"), None),
        P("ep", None, "tp"),
        P("ep", None, "tp"),
        P("ep", "tp", None),
    )
    return jax.shard_map(
        body,
        mesh=mesh,
        in_specs=placed,
        out_specs=(P(("ep", "tp"), None), P(("ep", "tp"), None)),
        check_vma=False,
    )
```

```python
import jax
import jax.numpy as jnp
from jax import lax
from jax.experimental import pallas as pl
from jax.experimental.pallas import tpu as pltpu
from jax.sharding import PartitionSpec as P
import functools

HEADS = 16
WINDOW = 128
GROUPS = 4


norm_eps = 1e-06
masked_score = -1e30


MESH = pl.DeviceIdType.MESH
CORES = 2
META = 128
HI = 32
LO = 64


def expert_kernel(
    dims, x_ref, gain_ref, sel_ref, meta_ref, q_ref, kv_ref, sink_ref, ow_ref,
    wg_hbm, wu_hbm, wd_hbm, mixed_ref, out_ref,
    wg, wu, wd, sbuf, buf, cbuf, xbuf, hbuf, wrow, pbuf, fb, sb, fin, ret,
    wsem, lsem, zs, zr, gs, gr, ps, pr, fs, fr, ss, sr, bs, br,
    kvx, att, mp, mq, mr, ks, kr, ms, mt, ns, nt, credit,
):
    planes, ranks, rows, per_block = dims
    tokens, width = x_ref.shape
    local = wg.shape[0]
    units = wg.shape[2]
    per_group = tokens // planes
    sides = rows
    ep, tp = lax.axis_index("ep"), lax.axis_index("tp")
    g, x = ep // ranks, ep % ranks
    y, c = tp // CORES, tp % CORES
    other = 1 - c
    part = pl.ds(0, width)

    def device(g_, x_, y_, c_):
        return (g_ * ranks + x_, y_ * CORES + c_)

    def x_peer(i):
        return lax.rem(x + i, ranks)

    def y_peer(j):
        return lax.rem(y + j, sides)

    loads = []
    for k, (h, v) in enumerate(((wg_hbm, wg), (wu_hbm, wu), (wd_hbm, wd))):
        cp = pltpu.make_async_copy(h, v, wsem.at[k])
        cp.start()
        loads.append(cp)

    barrier = pltpu.get_barrier_semaphore()
    friends = [device(lax.rem(g + d, planes), x, y, c) for d in range(1, planes)]
    friends += [device(g, x_peer(i), y, c) for i in range(1, ranks)]
    friends += [device(g, x, y_peer(j), c) for j in range(1, sides)]
    friends += [device(g, x, y, other)]
    ep_size = lax.axis_size("ep")
    after, ahead = lax.rem(ep + 1, ep_size), lax.rem(ep + ep_size - 1, ep_size)
    friends += [(after, tp), (ahead, tp)]
    for f in friends:
        pl.semaphore_signal(barrier, inc=1, device_id=f, device_id_type=MESH)

    values = x_ref[...].astype(jnp.float32)
    scale = lax.rsqrt(jnp.mean(values * values, axis=-1, keepdims=True) + norm_eps)
    normed = (values * scale * gain_ref[...]).astype(jnp.bfloat16)
    sel = sel_ref[...]
    ordered = jnp.dot(sel, normed, preferred_element_type=jnp.float32).astype(jnp.bfloat16)
    sbuf[:, :, :width] = ordered.reshape(planes, per_group, width)
    extra = jnp.dot(sel, meta_ref[...], preferred_element_type=jnp.float32).astype(jnp.bfloat16)
    sbuf[:, :, width:] = extra.reshape(planes, per_group, META)

    pl.semaphore_wait(barrier, len(friends))

    def remote(src, dst, s, r, dev):
        cp = pltpu.make_async_remote_copy(
            src_ref=src, dst_ref=dst, send_sem=s, recv_sem=r, device_id=dev, device_id_type=MESH
        )
        cp.start()
        return cp

    sent = []
    for d in range(1, planes):
        to = lax.rem(g + d, planes)
        sent.append(
            remote(sbuf.at[to], buf.at[d, c, x, y], zs.at[d], zr.at[d], device(to, x, y, c))
        )
    own = pltpu.make_async_copy(sbuf.at[g], buf.at[0, c, x, y], lsem)
    own.start()
    own.wait()
    seq = q_ref.shape[0]
    halos = [
        remote(kv_ref.at[pl.ds(seq - WINDOW, WINDOW)], kvx.at[pl.ds(0, WINDOW)], ks.at[0], kr.at[0], (after, tp)),
        remote(kv_ref.at[pl.ds(0, WINDOW)], kvx.at[pl.ds(seq + WINDOW, WINDOW)], ks.at[1], kr.at[1], (ahead, tp)),
    ]
    kvx[pl.ds(WINDOW, seq), :] = kv_ref[...]

    blocks = seq // WINDOW
    kv_local = kv_ref.shape[1] // META
    head_size = META // 2
    heads = q_ref.shape[1] // head_size

    def attention(n):
        qi = lax.broadcasted_iota(jnp.int32, (WINDOW, 3 * WINDOW), 0)
        ki = lax.broadcasted_iota(jnp.int32, (WINDOW, 3 * WINDOW), 1)
        distance = jnp.abs(ki - WINDOW - qi)
        place = ki + (ep * seq + (n - 1) * WINDOW)
        allowed = (distance <= WINDOW) & (place >= 0) & (place < seq * ep_size)
        apart = distance.astype(jnp.float32)
        outs = []
        for h in range(heads):
            at = h // (heads // kv_local) * META
            query = q_ref[n * WINDOW : (n + 1) * WINDOW, h * head_size : (h + 1) * head_size]
            near = kvx[n * WINDOW : (n + 3) * WINDOW, at : at + META]
            power = (tp * heads + h + 1).astype(jnp.float32) * (-8.0 / HEADS * 0.6931471805599453)
            slope = jnp.exp(jnp.full((1, 1), power, jnp.float32))
            scores = lax.dot_general(
                query, near[:, :head_size], (((1,), (1,)), ((), ())), preferred_element_type=jnp.float32
            ) * head_size ** (-0.5)
            scores = jnp.where(allowed, scores - slope * apart, masked_score)
            sink = sink_ref[:, h : h + 1]
            top = jnp.maximum(jnp.max(scores, axis=-1, keepdims=True), sink)
            grown = jnp.exp(scores - top)
            below = jnp.sum(grown, axis=-1, keepdims=True) + jnp.exp(sink - top)
            weights = (grown / below).astype(jnp.bfloat16)
            outs.append(jnp.dot(weights, near[:, head_size:], preferred_element_type=jnp.float32))
        att[n * WINDOW : (n + 1) * WINDOW, :] = jnp.concatenate(outs, axis=1).astype(jnp.bfloat16)

    def attend_share(k):
        if k == 0:
            for cp in halos:
                cp.wait_recv()
        for n in range(k * blocks // planes, (k + 1) * blocks // planes):
            attention(n)

    def mix():
        @pl.loop(0, width // 256)
        def _(k):
            cols = pl.ds(pl.multiple_of(k * 256, 256), 256)
            got = jnp.dot(att[...], ow_ref[:, cols], preferred_element_type=jnp.float32)
            mp[:, :, :, cols] = got.astype(jnp.bfloat16).reshape(*mp.shape[:3], 256)
        return [
            remote(mp.at[q, other], mq.at[q], ms.at[q], mt.at[q], device(g, x, y, other))
            for q in range(sides)
        ]

    def mix_hop(swapped):
        for q in range(sides):
            swapped[q].wait_recv()
            mp[q, c] = (mp[q, c].astype(jnp.float32) + mq[q].astype(jnp.float32)).astype(jnp.bfloat16)
        return [
            remote(mp.at[y_peer(j), c], mr.at[j - 1], ns.at[j - 1], nt.at[j - 1], device(g, x, y_peer(j), c))
            for j in range(1, sides)
        ]

    def mix_end(moved):
        total = mp[y, c].astype(jnp.float32)
        for j, cp in enumerate(moved):
            cp.wait_recv()
            total += mr[j].astype(jnp.float32)
        mixed_ref[...] = total.astype(jnp.bfloat16)

    counter = [0]

    def pass_on(d, bx, by, dev):
        block = buf.at[d, c, bx, by]
        sent.append(remote(block, block, gs.at[counter[0]], gr.at[d, c, bx, by], dev))
        counter[0] += 1

    def landed(d, bc, bx, by):
        block = buf.at[d, bc, bx, by]
        pltpu.make_async_remote_copy(
            src_ref=block, dst_ref=block, send_sem=gs.at[0], recv_sem=gr.at[d, bc, bx, by],
            device_id=device(g, x, y, other), device_id_type=MESH,
        ).wait_recv()

    def to_x(d, bx, by):
        for i in range(1, ranks):
            pass_on(d, bx, by, device(g, x_peer(i), y, c))

    def to_y(d, bx, by):
        for j in range(1, sides):
            pass_on(d, bx, by, device(g, x, y_peer(j), c))

    def to_core(d, bx, by):
        pass_on(d, bx, by, device(g, x, y, other))

    def spread(d):
        if d > 0:
            sent[d - 1].wait_recv()
        to_x(d, x, y)
        to_y(d, x, y)
        to_core(d, x, y)

    def relay(d):
        for i in range(1, ranks):
            landed(d, c, x_peer(i), y)
            if d % 2 == 0:
                to_y(d, x_peer(i), y)
            to_core(d, x_peer(i), y)
        for j in range(1, sides):
            landed(d, c, x, y_peer(j))
            if d % 2 == 1:
                to_x(d, x, y_peer(j))
            to_core(d, x, y_peer(j))

    def relay_far(d):
        for i in range(1, ranks):
            for j in range(1, sides):
                landed(d, c, x_peer(i), y_peer(j))
                to_core(d, x_peer(i), y_peer(j))

    def complete(d):
        for bx in range(ranks):
            for by in range(sides):
                landed(d, other, bx, by)

    spread(0)
    attend_share(0)
    for d in range(1, planes):
        spread(d)
        relay(d - 1)
        if d > 1:
            relay_far(d - 2)
        attend_share(d)
    swapped = mix()

    count = CORES * ranks * sides
    many = count * per_group
    slots = count * per_block
    stage = 2

    def gather_rows(first):
        ri = lax.broadcasted_iota(jnp.int32, (many, many), 0)
        ci = lax.broadcasted_iota(jnp.int32, (many, many), 1)
        lower = ((ci < ri) & (ci // per_group == ri // per_group)).astype(jnp.bfloat16)
        lane = lax.broadcasted_iota(jnp.int32, (many, META), 1)
        base = lax.broadcasted_iota(jnp.int32, (many, 1), 0) // per_group * per_block
        slot = lax.broadcasted_iota(jnp.int32, (many, slots), 1).astype(jnp.float32)
        lane_r = lax.broadcasted_iota(jnp.int32, (slots, META), 1)
        for s in range(stage):
            block = buf[first + s].reshape(many, width + META)
            marks = block[:, width:]
            ranks_in = jnp.dot(lower, marks, preferred_element_type=jnp.float32)
            for e in range(local):
                member = x * local + e
                mine = lane == member
                chosen = jnp.sum(jnp.where(mine, marks.astype(jnp.float32), 0.0), axis=1, keepdims=True)
                place = jnp.sum(jnp.where(mine, ranks_in, 0.0), axis=1, keepdims=True)
                place = place + base.astype(jnp.float32)
                hot = jnp.where((place == slot) & (chosen > 0.5), 1.0, 0.0).astype(jnp.bfloat16)
                cbuf[s, e] = hot
                picked = lax.dot_general(
                    hot, block, (((0,), (0,)), ((), ())), preferred_element_type=jnp.float32
                )
                xbuf[e, pl.ds(s * slots, slots), :] = picked[:, :width].astype(jnp.bfloat16)
                tail = picked[:, width:]
                weight = jnp.sum(
                    jnp.where((lane_r == member + HI) | (lane_r == member + LO), tail, 0.0),
                    axis=1, keepdims=True,
                )
                wrow[e, pl.ds(s * slots, slots), :] = jnp.broadcast_to(weight, (slots, META))

    tile = 256

    def hidden_of(e):
        @pl.loop(0, units // tile)
        def _(k):
            cols = pl.ds(pl.multiple_of(k * tile, tile), tile)
            xs = xbuf[e]
            a = jnp.dot(xs, wg[e, :, cols], preferred_element_type=jnp.float32)
            b = jnp.dot(xs, wu[e, :, cols], preferred_element_type=jnp.float32)
            act = a / (1.0 + jnp.exp(-a)) * b * wrow[e, :, :1]
            hbuf[e, :, cols] = act.astype(jnp.bfloat16)

    def project(first):
        @pl.loop(0, width // tile)
        def _(k):
            cols = pl.ds(pl.multiple_of(k * tile, tile), tile)
            outs = [
                jnp.dot(hbuf[e], wd[e, :, cols], preferred_element_type=jnp.float32).astype(jnp.bfloat16)
                for e in range(local)
            ]
            for s in range(stage):
                total = jnp.zeros((many, tile), jnp.float32)
                for e in range(local):
                    total += jnp.dot(
                        cbuf[s, e], outs[e][s * slots : (s + 1) * slots],
                        preferred_element_type=jnp.float32,
                    )
                buf[first + s, :, :, :, :, cols] = total.astype(jnp.bfloat16).reshape(
                    CORES, ranks, sides, per_group, tile
                )

    back = []
    pair, first_hop, second_hop, home = {}, {}, {}, {}

    def swap_cores(d):
        if d >= stage:
            pl.semaphore_wait(credit, 1)
        pair[d] = remote(
            buf.at[d, other, :, :, :, part], pbuf.at[d % stage], ps.at[d], pr.at[d], device(g, x, y, other)
        )

    def hop_one(d):
        pair[d].wait_recv()
        for bx in range(ranks):
            for by in range(sides):
                buf[d, c, bx, by, :, part] = (
                    buf[d, c, bx, by, :, part].astype(jnp.float32) + pbuf[d % stage, bx, by].astype(jnp.float32)
                ).astype(jnp.bfloat16)
        if d < planes - stage:
            pl.semaphore_signal(credit, inc=1, device_id=device(g, x, y, other), device_id_type=MESH)
        first_hop[d] = []
        along_y = d % 2 == 0
        for j in range(1, sides if along_y else ranks):
            for q in range(ranks if along_y else sides):
                if along_y:
                    src, dev = buf.at[d, c, q, y_peer(j), :, part], device(g, x, y_peer(j), c)
                else:
                    src, dev = buf.at[d, c, x_peer(j), q, :, part], device(g, x_peer(j), y, c)
                first_hop[d].append(
                    remote(src, fb.at[d, j - 1, q], fs.at[d, j - 1, q], fr.at[d, j - 1, q], dev)
                )

    def hop_two(d):
        for cp in first_hop[d]:
            cp.wait_recv()
        along_y = d % 2 == 0
        for q in range(ranks if along_y else sides):
            here = (d, c, q, y) if along_y else (d, c, x, q)
            total = buf[(*here, slice(None), part)].astype(jnp.float32)
            for j in range(1, sides if along_y else ranks):
                total += fb[d, j - 1, q].astype(jnp.float32)
            buf[(*here, slice(None), part)] = total.astype(jnp.bfloat16)
        second_hop[d] = []
        for i in range(1, ranks if along_y else sides):
            if along_y:
                src, dev = buf.at[d, c, x_peer(i), y, :, part], device(g, x_peer(i), y, c)
            else:
                src, dev = buf.at[d, c, x, y_peer(i), :, part], device(g, x, y_peer(i), c)
            second_hop[d].append(remote(src, sb.at[d, i - 1], ss.at[d, i - 1], sr.at[d, i - 1], dev))

    def go_home(d):
        for cp in second_hop[d]:
            cp.wait_recv()
        total = buf[d, c, x, y, :, part].astype(jnp.float32)
        for i in range(len(second_hop[d])):
            total += sb[d, i].astype(jnp.float32)
        if d == 0:
            ret[g] = total.astype(jnp.bfloat16)
        else:
            fin[d] = total.astype(jnp.bfloat16)
            to = lax.rem(g + planes - d, planes)
            home[d] = remote(fin.at[d], ret.at[g], bs.at[d], br.at[d], device(to, x, y, c))

    for first in range(0, planes, stage):
        ds = range(first, first + stage)
        before = range(first - stage, first) if first else ()
        for d in ds:
            complete(d)
        gather_rows(first)
        if not first:
            relay(planes - 1)
            relay_far(planes - 2)
            loads[0].wait()
            loads[1].wait()
        for d in before:
            hop_one(d)
        for e in range(local):
            hidden_of(e)
            if e == 0:
                for d in before:
                    hop_two(d)
                if not first:
                    relay_far(planes - 1)
                    moved = mix_hop(swapped)
        for d in before:
            go_home(d)
        if not first:
            loads[2].wait()
            for cp in sent:
                cp.wait_send()
        project(first)
        for d in ds:
            swap_cores(d)
    mix_end(moved)
    for d in ds:
        hop_one(d)
    for d in ds:
        hop_two(d)
    for d in ds:
        go_home(d)
    for cp in halos + swapped + moved:
        cp.wait_send()
    for d in range(planes):
        pair[d].wait_send()
        for cp in first_hop[d] + second_hop[d]:
            cp.wait_send()
    for d in range(1, planes):
        home[d].wait_send()
        came = lax.rem(g + d, planes)
        pltpu.make_async_remote_copy(
            src_ref=fin.at[d], dst_ref=ret.at[came], send_sem=bs.at[d], recv_sem=br.at[d],
            device_id=device(came, x, y, c), device_id_type=MESH,
        ).wait_recv()
    out_ref[...] = lax.dot_general(
        sel_ref[...], ret[...].reshape(tokens, width), (((0,), (0,)), ((), ())),
        preferred_element_type=jnp.float32,
    ).astype(jnp.bfloat16)


def both_of(
    queries, keys_values, sink_logits, out_weight,
    expert_input, norm_gain, route_group, route_expert, group_logits, expert_logits,
    gate_weight, up_weight, down_weight,
):
    ep_size, tp_size = lax.axis_size("ep"), lax.axis_size("tp")
    tokens, width = expert_input.shape
    local, _, units = gate_weight.shape
    planes, ranks, sides = GROUPS, ep_size // GROUPS, tp_size // CORES
    members = local * ranks
    per_group = tokens // planes
    chosen = route_expert.shape[1]
    per_block = per_group * chosen // members
    slots = CORES * ranks * sides * per_block
    many = CORES * ranks * sides * per_group
    ids = jnp.arange(tokens, dtype=jnp.int32)
    same = (route_group[:, None] == route_group[None, :]) & (ids[:, None] < ids[None, :])
    place = route_group * per_group + jnp.sum(same.astype(jnp.int32), axis=0)
    sel = (place[None, :] == ids[:, None]).astype(jnp.bfloat16)
    group_exp = jnp.exp(group_logits)
    groups = jnp.arange(GROUPS, dtype=jnp.int32)[None, :]
    picked = jnp.sum(jnp.where(groups == route_group[:, None], group_exp, 0.0), axis=1) / jnp.sum(
        group_exp, axis=1
    )
    member_exp = jnp.exp(expert_logits)
    weight = member_exp / jnp.sum(member_exp, axis=1, keepdims=True) * picked[:, None]
    high = lax.reduce_precision(weight, 8, 7)
    low = weight - high
    lane = jnp.arange(META, dtype=jnp.int32)[None, :]
    meta = jnp.zeros((tokens, META), jnp.float32)
    for k in range(chosen):
        at = route_expert[:, k : k + 1]
        meta = meta + jnp.where(lane == at, 1.0, 0.0)
        meta = meta + jnp.where(lane == at + HI, high[:, k : k + 1], 0.0)
        meta = meta + jnp.where(lane == at + LO, low[:, k : k + 1], 0.0)
    bf16, dma = jnp.bfloat16, pltpu.SemaphoreType.DMA
    most, wide = max(ranks, sides), max(ranks, sides, 2) - 1
    sends = planes * (ranks * sides * 3)
    vmem = pl.BlockSpec(memory_space=pltpu.VMEM)
    hbm = pl.BlockSpec(memory_space=pl.ANY)
    rows = 2 * slots
    seq = queries.shape[0]
    kv = keys_values.reshape(seq, -1)
    share = seq // tp_size
    return pl.pallas_call(
        functools.partial(expert_kernel, (planes, ranks, sides, per_block)),
        out_shape=(jax.ShapeDtypeStruct((share, width), bf16), jax.ShapeDtypeStruct((tokens, width), bf16)),
        in_specs=[vmem] * 8 + [hbm] * 3,
        out_specs=(vmem, vmem),
        scratch_shapes=[
            pltpu.VMEM(gate_weight.shape, bf16),
            pltpu.VMEM(up_weight.shape, bf16),
            pltpu.VMEM(down_weight.shape, bf16),
            pltpu.VMEM((planes, per_group, width + META), bf16),
            pltpu.VMEM((planes, CORES, ranks, sides, per_group, width + META), bf16),
            pltpu.VMEM((2, local, many, slots), bf16),
            pltpu.VMEM((local, rows, width), bf16),
            pltpu.VMEM((local, rows, units), bf16),
            pltpu.VMEM((local, rows, META), jnp.float32),
            pltpu.VMEM((2, ranks, sides, per_group, width), bf16),
            pltpu.VMEM((planes, wide, most, per_group, width), bf16),
            pltpu.VMEM((planes, wide, per_group, width), bf16),
            pltpu.VMEM((planes, per_group, width), bf16),
            pltpu.VMEM((planes, per_group, width), bf16),
            dma((3,)), dma,
            dma((planes,)), dma((planes,)),
            dma((sends,)), dma((planes, CORES, ranks, sides)),
            dma((planes,)), dma((planes,)),
            dma((planes, wide, most)), dma((planes, wide, most)),
            dma((planes, wide)), dma((planes, wide)),
            dma((planes,)), dma((planes,)),
            pltpu.VMEM((seq + 2 * WINDOW, kv.shape[1]), bf16),
            pltpu.VMEM(queries.shape, bf16),
            pltpu.VMEM((sides, CORES, share, width), bf16),
            pltpu.VMEM((sides, share, width), bf16),
            pltpu.VMEM((sides - 1, share, width), bf16),
            dma((2,)), dma((2,)), dma((sides,)), dma((sides,)), dma((sides - 1,)), dma((sides - 1,)),
            pltpu.SemaphoreType.REGULAR,
        ],
        compiler_params=pltpu.CompilerParams(
            collective_id=0, has_side_effects=True, vmem_limit_bytes=KERNEL_VMEM
        ),
        cost_estimate=pl.CostEstimate(
            flops=6 * 2 * rows * local * width * units, bytes_accessed=6 * local * width * units, transcendentals=0
        ),
    )(expert_input, norm_gain[None, :], sel, meta.astype(bf16), queries, kv, sink_logits[None, :], out_weight, gate_weight, up_weight, down_weight)


KERNEL_VMEM = 67_043_328


def body(
    queries,
    keys_values,
    sink_logits,
    out_weight,
    expert_input,
    norm_gain,
    route_group,
    route_expert,
    group_logits,
    expert_logits,
    gate_weight,
    up_weight,
    down_weight,
):
    return both_of(
        queries, keys_values, sink_logits, out_weight,
        expert_input, norm_gain, route_group, route_expert, group_logits, expert_logits,
        gate_weight, up_weight, down_weight,
    )


def solution(mesh):
    placed = (
        P("ep", "tp"),
        P("ep", "tp", None),
        P("tp"),
        P("tp", None),
        P(("ep", "tp"), None),
        P(),
        P(("ep", "tp")),
        P(("ep", "tp"), None),
        P(("ep", "tp"), None),
        P(("ep", "tp"), None),
        P("ep", None, "tp"),
        P("ep", None, "tp"),
        P("ep", "tp", None),
    )
    return jax.shard_map(
        body,
        mesh=mesh,
        in_specs=placed,
        out_specs=(P(("ep", "tp"), None), P(("ep", "tp"), None)),
        check_vma=False,
    )
```
